32 devices in a mesh: sp: 8 (over z, y), tp: 4 (over x, core).
Axes of the slice: x: 2, y: 2, z: 4, core: 2. Of those that a mesh axis runs over, the one named last changes fastest.
Arguments:
- tokens: bfloat16 [2048, 4096], P(('sp', 'tp')), may hold values from -6 to 6, as said below
- query_one: bfloat16 [4096, 1024], P('sp', 'tp'), may hold values from -0.125 to 0.125
- query_two: bfloat16 [4096, 1024], P('sp', 'tp'), may hold values from -0.125 to 0.125
- key_one: bfloat16 [4096, 1024], P('sp', 'tp'), may hold values from -0.125 to 0.125
- key_two: bfloat16 [4096, 1024], P('sp', 'tp'), may hold values from -0.125 to 0.125
- value_weight: bfloat16 [4096, 2048], P('sp', 'tp'), may hold values from -0.09375 to 0.09375
- out_weight: bfloat16 [2048, 4096], P('tp', 'sp'), may hold values from -0.125 to 0.125
- lambdas: float32 [8], P('tp'), may hold values from 0.3 to 0.8
- head_gain: float32 [256], replicated, may hold values from 0.1 to 1.9
Outputs:
- layer_out: bfloat16 [2048, 4096], P(('sp', 'tp'))
The draws below stay inside these ranges and needn't reach their ends.
Inputs may be any that keep to these rules, and one draw needn't show every extreme that they name: `tokens`: the features' mean changes between 16 equal spans of the sequence.
All inputs are finite; a program needn't handle non-finite values.
Results may differ from the reference program's by a relative error of at most 0.013.
The reference program's roundings to bfloat16 on the way count: a program that leaves them out, or rounds other values in their place, can miss the bound.
Values may be sent and summed in bfloat16 or wider, within the bound.
No kernel may reach another device: no remote copies, remote signals or barrier semaphores. Data moves between devices by JAX's collectives and lax.ppermute only.
A program may use at most 128 MiB of HBM per device.

```python
import jax
import jax.numpy as jnp
from jax import lax

D = 4096
H = 8
QK = 128
V = 256
TOK_DEV = 256
TOKENS = 2048


def draw_tokens(key, part):
    base_key, mean_key, row_key = jax.random.split(key, 3)
    span_ids = jnp.arange(TOKENS, dtype=jnp.int32) * 16 // TOKENS
    span_means = 0.6 * jnp.clip(jax.random.normal(mean_key, (16, D), jnp.float32), -2.5, 2.5)
    offsets = span_means[span_ids]
    base_draw = jnp.clip(jax.random.normal(base_key, (TOKENS, D), jnp.float32), -4.5, 4.5)
    values = jnp.clip(base_draw + offsets, -6.0, 6.0)
    return values.astype(jnp.bfloat16)


def block_scale(own_key, dims, cuts, smallest, high):
    gain = 1.0
    for dim, parts in cuts:
        heights = jax.random.uniform(jax.random.fold_in(jax.random.fold_in(own_key, 6), dim), (parts,), jnp.float32, smallest / len(cuts), high / len(cuts))
        gain = gain * jnp.repeat(jnp.exp(heights), dims[dim] // parts).reshape((-1,) + (1,) * (len(dims) - 1 - dim))
    return gain


def scatter_about(key, dims, scale, limit, cuts=(), held_as=jnp.bfloat16):
    values = jax.random.normal(key, dims, jnp.float32) * scale
    if len(cuts) > 0:
        values = block_scale(key, dims, cuts, -0.22, 0.18) * values
    return jnp.clip(values, min=-limit, max=limit).astype(held_as)


def setup_inputs(seed: int = 0) -> dict:
    keys = jax.random.split(jax.random.key(seed), 10)
    tokens = draw_tokens(jax.random.fold_in(keys[9], 71), 0)
    query_one = scatter_about(keys[1], (D, H * QK), (D * 4 // 7) ** -0.5, 0.125, ((0, 8), (1, 4)))
    query_two = scatter_about(keys[2], (D, H * QK), (D * 4 // 7) ** -0.5, 0.125, ((0, 8), (1, 4)))
    key_one = scatter_about(keys[3], (D, H * QK), (D * 4 // 7) ** -0.5, 0.125, ((0, 8), (1, 4)))
    key_two = scatter_about(keys[4], (D, H * QK), (D * 4 // 7) ** -0.5, 0.125, ((0, 8), (1, 4)))
    value_weight = scatter_about(keys[5], (D, H * V), D ** -0.5, 0.09375, ((0, 8), (1, 4)))
    out_weight = scatter_about(keys[6], (H * V, D), (H * V) ** -0.5, 0.125, ((0, 4), (1, 8)))
    lambdas = jnp.clip(0.3 + 0.5 * jax.random.uniform(keys[7], (H,), jnp.float32) ** block_scale(keys[7], (H,), ((0, 4),), -0.2, 0.2), 0.3, 0.8)
    head_gain = jnp.clip(1.0 + 0.18 * jax.random.normal(keys[8], (V,), jnp.float32), 0.1, 1.9)
    return dict(tokens=tokens, query_one=query_one, query_two=query_two, key_one=key_one, key_two=key_two, value_weight=value_weight, out_weight=out_weight, lambdas=lambdas, head_gain=head_gain)


ROPE_BASE = 500000.0
EPS_NORM = 0.02

def rotate(values, positions):
    half_dim = values.shape[-1] // 2
    inverse = 1.0 / ROPE_BASE ** (jnp.arange(0, 2 * half_dim, 2, dtype=jnp.float32) / (2 * half_dim))
    angles = positions.astype(jnp.float32)[:, None] * inverse[None, :]
    cos_part = jnp.cos(angles)[:, None, :]
    sin_part = jnp.sin(angles)[:, None, :]
    first_half = values[..., :half_dim]
    second_half = values[..., half_dim:]
    return jnp.concatenate([first_half * cos_part - second_half * sin_part, second_half * cos_part + first_half * sin_part], axis=-1)

def reference(tokens, query_one, query_two, key_one, key_two, value_weight, out_weight, lambdas, head_gain):
    seq_len = tokens.shape[0]
    positions = jnp.arange(seq_len, dtype=jnp.int32)

    def project(weight):
        product = jnp.dot(tokens, weight, preferred_element_type=jnp.float32)
        return rotate(product.reshape(seq_len, H, QK), positions).astype(jnp.bfloat16)
    q_one = project(query_one)
    q_two = project(query_two)
    k_one = project(key_one)
    k_two = project(key_two)
    values = jnp.dot(tokens, value_weight, preferred_element_type=jnp.float32).astype(jnp.bfloat16)
    values = values.reshape(seq_len, H, V).astype(jnp.float32)
    block_len = TOK_DEV
    n_blocks = seq_len // block_len

    def one_block(block_index):
        start_row = block_index * block_len
        q_pos = start_row + jnp.arange(block_len, dtype=jnp.int32)
        allowed = positions[None, :] <= q_pos[:, None]
        map_outs = []
        for q_all, k_all in ((q_one, k_one), (q_two, k_two)):
            q_blk = lax.dynamic_slice_in_dim(q_all, start_row, block_len, 0)
            scores = jnp.einsum('qhd,khd->hqk', q_blk.astype(jnp.float32), k_all.astype(jnp.float32)) * QK ** (-0.5)
            masked = jnp.where(allowed[None], scores, -1e+30)
            row_top = lax.optimization_barrier(jnp.max(masked, axis=-1, keepdims=True))
            exp_weights = jnp.where(allowed[None], jnp.exp(scores - row_top), 0.0)
            row_total = lax.optimization_barrier(jnp.sum(exp_weights, axis=-1))
            rounded = lax.optimization_barrier(exp_weights.astype(jnp.bfloat16))
            weighted = jnp.einsum('hqk,khv->hqv', rounded.astype(jnp.float32), values)
            map_outs.append(weighted / row_total[..., None])
        mixed_out = map_outs[0] - lambdas[:, None, None] * map_outs[1]
        scaled = mixed_out * lax.rsqrt(lax.optimization_barrier(jnp.mean(mixed_out * mixed_out, axis=-1, keepdims=True)) + EPS_NORM) * head_gain
        return jnp.transpose(scaled, (1, 0, 2)).reshape(block_len, H * V).astype(jnp.bfloat16)
    attended = lax.map(one_block, jnp.arange(n_blocks, dtype=jnp.int32)).reshape(seq_len, H * V)
    return jnp.dot(attended, out_weight, preferred_element_type=jnp.float32).astype(jnp.bfloat16)
```

```python
import functools

import jax
import jax.numpy as jnp
from jax import lax
from jax.experimental import pallas as pl
from jax.experimental.pallas import tpu as pltpu
from jax.sharding import PartitionSpec as P

ROPE_BASE = 500000.0
EPS_NORM = 0.02
MASKED = -1e30
LOG2_E = 1.4426950408889634


SMEM = pl.BlockSpec(memory_space=pltpu.SMEM)
VMEM = pl.BlockSpec(memory_space=pltpu.VMEM)


def sweep(low, high, body, carry):
    if high - low <= 4:
        for i in range(low, high):
            carry = body(i, carry)
        return carry
    return lax.fori_loop(low, high, body, carry)


def pack_kernel(dims, place, q1, q2, k1, k2, v, keep, give):
    nc, hp, qk, v_dim = dims
    z, c = place[0], place[3]
    half = v_dim // nc
    for own_core in range(nc):

        @pl.when(c == own_core)
        def _():
            for target, ref in ((own_core, keep), (1 - own_core, give)):
                q, k = ((q1, k1), (q2, k2))[target]
                for b in range(hp):
                    slot = jnp.bitwise_xor(lax.rem(z, hp), b)
                    ref[slot, :, :qk] = q[:, b * qk : (b + 1) * qk]
                    ref[slot, :, qk : 2 * qk] = k[:, b * qk : (b + 1) * qk]
                    low = b * v_dim + target * half
                    ref[slot, :, 2 * qk :] = v[:, low : low + half]


def project_kernel(dims, place, cos_ref, sin_ref, *refs):
    nz, ny, nx, nc, rows, depth, qk, windows = dims
    tokens = refs[: nz * nx]
    weights = refs[nz * nx : nz * nx + nz * ny * nc]
    out_ref, acc = refs[nz * nx + nz * ny * nc :]
    z, y = place[0], place[1]
    low, high = windows[0][0], windows[-1][1]
    wide = high - low
    for r in range(nz):
        for ky in range(ny):
            start = (jnp.bitwise_xor(z, r) * ny + lax.rem(y + ky, ny)) * depth
            cols = pl.ds(pl.multiple_of(start, depth), depth)
            left = jnp.concatenate([t[:, cols] for t in tokens], axis=0)
            for kc in range(nc):
                right = weights[(r * ny + ky) * nc + kc][:, low:high]
                part = jnp.dot(left, right, preferred_element_type=jnp.float32)
                if r or ky:
                    part = part + acc[kc]
                acc[kc] = part
    half = qk // 2
    at = 0
    for first, last, rotated in windows:
        for kc in range(nc):
            value = acc[kc, :, first - low : last - low]
            if rotated:
                a, b = value[:, :half], value[:, half:]
                cos, sin = cos_ref[...], sin_ref[...]
                value = jnp.concatenate([a * cos - b * sin, b * cos + a * sin], axis=1)
            out_ref[:, at : at + last - first] = value.astype(jnp.bfloat16)
            at += last - first


def attend_kernel(dims, place, q_ref, lam_ref, gain_ref, *refs):
    nz, ny, nx, nc, rows, qk, v = dims
    pieces = refs[: ny * nc]
    out_ref, kv_all, s_all = refs[ny * nc :]
    z, y, x, c = (place[i] for i in range(4))
    tile = nx * rows
    block = ny * nc * tile
    half = v // nc
    for ky in range(ny):
        for kc in range(nc):
            piece = pieces[ky * nc + kc]
            slot = lax.rem(y + ky, ny) * nc + lax.rem(c + kc, nc)
            for r in range(nz):
                start = (jnp.bitwise_xor(z, r) * (ny * nc) + slot) * tile
                to = pl.ds(pl.multiple_of(start, tile), tile)
                part = piece[r * tile : (r + 1) * tile, :]
                for m in range(nc):
                    n = (m + kc) % nc
                    kv_all[to, n * qk : (n + 1) * qk] = part[:, m * qk : (m + 1) * qk]
                    kv_all[to, nc * qk + n * half : nc * qk + (n + 1) * half] = part[
                        :, nc * qk + m * half : nc * qk + (m + 1) * half
                    ]

    def offset(index, y_at, c_at):
        x_at = lax.rem(x + index // rows, nx)
        return (y_at * nx + x_at) * nc * rows + c_at * rows + index % rows

    chunk = min(block, 512)
    each = block // chunk
    q_off = offset(lax.broadcasted_iota(jnp.int32, (tile, 1), 0), y, c)
    k_index = lax.broadcasted_iota(jnp.int32, (1, chunk), 1)
    factor = qk ** (-0.5) * LOG2_E

    def key_rows(j):
        return pl.ds(pl.multiple_of(j * chunk, chunk), chunk)

    for t in range(nz):
        q_start = pl.multiple_of(jnp.bitwise_xor(z, t) * tile, tile)
        outs = []
        for m in range(nc):
            q = q_ref[pl.ds(q_start, tile), m * qk : (m + 1) * qk]

            def scores(j, top, masked):
                keys = kv_all[key_rows(j), m * qk : (m + 1) * qk]
                s = lax.dot_general(
                    q, keys, (((1,), (1,)), ((), ())), preferred_element_type=jnp.float32
                )
                if masked:
                    index = k_index + (j - t * each) * chunk
                    slot = index // tile
                    k_off = offset(index % tile, slot // nc, slot % nc)
                    s = jnp.where(k_off <= q_off, s, MASKED)
                s_all[:, key_rows(j)] = s
                return jnp.maximum(top, jnp.max(s, axis=-1, keepdims=True))

            top = jnp.full((tile, 1), MASKED, jnp.float32)
            top = sweep(0, t * each, lambda j, v_: scores(j, v_, False), top)
            top = sweep(t * each, (t + 1) * each, lambda j, v_: scores(j, v_, True), top)

            def gather(j, carry):
                total, acc = carry
                e = jnp.exp2((s_all[:, key_rows(j)] - top) * factor)
                total = total + jnp.sum(e, axis=-1, keepdims=True)
                vals = kv_all[key_rows(j), nc * qk :]
                acc = acc + jnp.dot(
                    e.astype(jnp.bfloat16), vals, preferred_element_type=jnp.float32
                )
                return total, acc

            total, acc = sweep(
                0,
                (t + 1) * each,
                gather,
                (jnp.zeros((tile, 1), jnp.float32), jnp.zeros((tile, v), jnp.float32)),
            )
            outs.append(acc / total)
        one = jnp.where(c == 0, outs[0], outs[1])
        two = jnp.where(c == 0, outs[1], outs[0])
        mixed = one - lam_ref[0] * two
        mixed = jnp.where(
            c == 0, mixed, jnp.concatenate([mixed[:, half:], mixed[:, :half]], axis=1)
        )
        mean = jnp.mean(mixed * mixed, axis=-1, keepdims=True)
        scaled = mixed * lax.rsqrt(mean + EPS_NORM) * gain_ref[...]
        out_ref[t * tile : (t + 1) * tile, :] = scaled.astype(jnp.bfloat16)


def out_kernel(dims, place, *refs):
    nz, ny, nx, nc, hp, v = dims
    chunks = refs[:nz]
    weights = refs[nz : nz + nx * ny * nc]
    out_ref, heads = refs[nz + nx * ny * nc :]
    z, y, c = place[0], place[1], place[3]
    count = chunks[0].shape[0]
    cols = weights[0].shape[1]
    for r in range(nz):
        for kx in range(nx):
            heads[kx, r] = chunks[r][:, kx * v : (kx + 1) * v]
    for ky in range(ny):
        total = jnp.zeros((count, cols), jnp.float32)
        for kx in range(nx):
            for kc in range(nc):
                for b in range(hp):
                    r = jnp.bitwise_xor(lax.rem(c + kc, nc) * hp + b, z)
                    total += jnp.dot(
                        heads[kx, r],
                        weights[(kx * ny + ky) * nc + kc][b * v : (b + 1) * v, :],
                        preferred_element_type=jnp.float32,
                    )
        to = pl.multiple_of(lax.rem(y + ky, ny) * cols, cols)
        out_ref[:, pl.ds(to, cols)] = total.astype(jnp.bfloat16)


def on_device(
    nx,
    tokens,
    query_one,
    query_two,
    key_one,
    key_two,
    value_weight,
    out_weight,
    lambdas,
    head_gain,
):
    sp, tp = lax.axis_size("sp"), lax.axis_size("tp")
    nc = tp // nx
    hp = lambdas.shape[0]
    nz = hp * nc
    ny = sp // nz
    rows = tokens.shape[0]
    span = rows * tp
    depth = query_one.shape[0]
    qk = query_one.shape[1] // hp
    v = value_weight.shape[1] // hp
    half = v // nc
    share = 2 * qk + half
    sp_at, tp_at = lax.axis_index("sp"), lax.axis_index("tp")
    z, y = sp_at // ny, sp_at % ny
    x, c = tp_at // nc, tp_at % nc
    place = jnp.stack([z, y, x, c]).astype(jnp.int32)

    def send(value, where, only=None):
        pairs = []
        for a in range(nz):
            for b in range(ny):
                for d in range(nx):
                    for e in range(nc):
                        if only is not None and a not in only:
                            continue
                        to = where(a, b, d, e)
                        pairs.append(
                            (
                                (a * ny + b) * tp + d * nc + e,
                                (to[0] * ny + to[1]) * tp + to[2] * nc + to[3],
                            )
                        )
        return lax.ppermute(value, ("sp", "tp"), pairs)

    def from_z(value, r):
        return send(value, lambda a, b, d, e: (a ^ r, b, d, e)) if r else value

    def from_y(value, k):
        return send(value, lambda a, b, d, e: (a, (b - k) % ny, d, e)) if k else value

    def from_x(value, k):
        return send(value, lambda a, b, d, e: (a, b, (d - k) % nx, e)) if k else value

    def from_c(value, k):
        return send(value, lambda a, b, d, e: (a, b, d, (e - k) % nc)) if k else value

    if nz == 4:
        mid = (1, 2)
        near = from_z(tokens, 1)
        cross = send(tokens, lambda a, b, d, e: (3 - a, b, d, e), mid)
        out_two = send(cross, lambda a, b, d, e: (a ^ 1, b, d, e), mid)
        mid_two = send(near, lambda a, b, d, e: (3 - a, b, d, e), mid)
        out_three = send(mid_two, lambda a, b, d, e: (a ^ 1, b, d, e), mid)
        in_mid = (z == 1) | (z == 2)
        spans = [
            tokens,
            near,
            jnp.where(in_mid, mid_two, out_two),
            jnp.where(in_mid, cross, out_three),
        ]
    else:
        spans = [from_z(tokens, r) for r in range(nz)]
    token_pieces = [from_x(spans[r], k) for r in range(nz) for k in range(nx)]

    shares = jax.ShapeDtypeStruct((hp, depth, share), jnp.bfloat16)
    keep, give = pl.pallas_call(
        functools.partial(pack_kernel, (nc, hp, qk, v)),
        out_shape=(shares, shares),
        in_specs=[SMEM] + [VMEM] * 5,
        out_specs=(VMEM, VMEM),
        cost_estimate=pl.CostEstimate(
            flops=8 * depth * share * hp, bytes_accessed=8 * depth * share * hp, transcendentals=0
        ),
        name="pack",
    )(place, query_one, query_two, key_one, key_two, value_weight)
    taken = from_c(give, 1)
    weight_pieces = []
    for r in range(nz):
        owner = (z ^ r) // hp
        mine = jnp.where(owner == c, keep[r % hp], taken[r % hp])
        got = from_z(mine, r)
        for ky in range(ny):
            beside = from_y(got, ky)
            for kc in range(nc):
                weight_pieces.append(from_c(beside, kc))

    index = jnp.arange(nz * nx * rows, dtype=jnp.int32)
    at_z = z ^ (index // (nx * rows))
    at_x = (x + (index // rows) % nx) % nx
    positions = (at_z * ny + y) * span + (at_x * nc + c) * rows + index % rows
    turn = qk // 2
    inverse = 1.0 / ROPE_BASE ** (jnp.arange(0, 2 * turn, 2, dtype=jnp.float32) / (2 * turn))
    angles = positions.astype(jnp.float32)[:, None] * inverse[None, :]
    cos_part, sin_part = jnp.cos(angles), jnp.sin(angles)

    total_rows = nz * nx * rows

    def project(windows, name):
        wide = sum(last - first for first, last, _ in windows)
        return pl.pallas_call(
            functools.partial(project_kernel, (nz, ny, nx, nc, rows, depth, qk, windows)),
            out_shape=jax.ShapeDtypeStruct((total_rows, nc * wide), jnp.bfloat16),
            in_specs=[SMEM] + [VMEM] * (2 + nz * nx + nz * ny * nc),
            out_specs=VMEM,
            scratch_shapes=[pltpu.VMEM((nc, total_rows, wide), jnp.float32)],
            cost_estimate=pl.CostEstimate(
                flops=2 * total_rows * sp * depth * nc * wide,
                bytes_accessed=2 * sp * depth * (total_rows + nc * wide),
                transcendentals=0,
            ),
            name=name,
        )(place, cos_part, sin_part, *token_pieces, *weight_pieces)

    kv = project(((qk, 2 * qk, True), (2 * qk, share, False)), "project_kv")
    kv_pieces = []
    for ky in range(ny):
        beside = from_y(kv, ky)
        for kc in range(nc):
            kv_pieces.append(from_c(beside, kc))
    q = project(((0, qk, True),), "project_q")

    out_pieces = []
    for kx in range(nx):
        over = from_x(out_weight, kx)
        for ky in range(ny):
            beside = from_y(over, ky)
            for kc in range(nc):
                out_pieces.append(from_c(beside, kc))

    lam_all = jnp.stack([from_c(lambdas, k) for k in range(nc)])
    lam = lax.dynamic_slice(lam_all, ((z // hp - c) % nc, z % hp), (1, 1))
    pairs = total_rows * total_rows * ny * nc
    attended = pl.pallas_call(
        functools.partial(attend_kernel, (nz, ny, nx, nc, rows, qk, v)),
        out_shape=jax.ShapeDtypeStruct((total_rows, v), jnp.bfloat16),
        in_specs=[SMEM, VMEM, SMEM, VMEM] + [VMEM] * (ny * nc),
        out_specs=VMEM,
        scratch_shapes=[
            pltpu.VMEM((ny * nc * total_rows, 2 * qk + v), jnp.bfloat16),
            pltpu.VMEM((nx * rows, ny * nc * total_rows), jnp.float32),
        ],
        cost_estimate=pl.CostEstimate(
            flops=4 * pairs * (qk + v),
            bytes_accessed=2 * ny * nc * total_rows * (2 * qk + v),
            transcendentals=2 * pairs,
        ),
        name="attend",
    )(place, q, lam.reshape(1), head_gain.reshape(1, v), *kv_pieces)

    attended = attended.reshape(nz, nx, rows, v)
    own = jnp.concatenate(
        [from_x(attended[:, (nx - k) % nx], k).reshape(nz * rows, v) for k in range(nx)], axis=1
    )
    chunks = [from_z(own, r) for r in range(nz)]
    cols = ny * out_weight.shape[1]
    result = pl.pallas_call(
        functools.partial(out_kernel, (nz, ny, nx, nc, hp, v)),
        out_shape=jax.ShapeDtypeStruct((nz * rows, cols), jnp.bfloat16),
        in_specs=[SMEM] + [VMEM] * (nz + nx * ny * nc),
        out_specs=VMEM,
        scratch_shapes=[pltpu.VMEM((nx, nz, nz * rows, v), jnp.bfloat16)],
        cost_estimate=pl.CostEstimate(
            flops=2 * nz * rows * nx * nz * v * cols,
            bytes_accessed=2 * nx * nz * v * cols,
            transcendentals=0,
        ),
        name="out_project",
    )(place, *chunks, *out_pieces)
    out = jnp.zeros((rows, nz * cols), jnp.bfloat16)
    for r in range(nz):
        mine = lax.dynamic_slice_in_dim(result, (z ^ r) * rows, rows, axis=0)
        out = lax.dynamic_update_slice(out, from_z(mine, r), (0, (z ^ r) * cols))
    return out


def solution(mesh):
    in_specs = (
        P(("sp", "tp"), None),
        P("sp", "tp"),
        P("sp", "tp"),
        P("sp", "tp"),
        P("sp", "tp"),
        P("sp", "tp"),
        P("tp", "sp"),
        P("tp"),
        P(),
    )
    out_specs = P(("sp", "tp"), None)
    return jax.shard_map(
        functools.partial(on_device, 2),
        mesh=mesh,
        in_specs=in_specs,
        out_specs=out_specs,
        check_vma=False,
    )
```

```python
import functools
import math

import jax
import jax.numpy as jnp
from jax import lax
from jax.experimental import pallas as pl
from jax.experimental.pallas import tpu as pltpu
from jax.sharding import PartitionSpec as P


ROPE_BASE = 500000.0
EPS_NORM = 0.02
MASKED = -1e30
LOG2_E = 1.4426950408889634


SMEM = pl.BlockSpec(memory_space=pltpu.SMEM)
VMEM = pl.BlockSpec(memory_space=pltpu.VMEM)


def room(*shapes):
    held = sum(math.prod(shape) * size for shape, size in shapes)
    return pltpu.CompilerParams(vmem_limit_bytes=min(60 << 20, held + held // 4 + (3 << 20)))


def sweep(low, high, body, carry):
    if high - low <= 4:
        for i in range(low, high):
            carry = body(i, carry)
        return carry
    return lax.fori_loop(low, high, body, carry)


def pack_kernel(dims, place, q1, q2, k1, k2, v, keep, give):
    nc, hp, qk, v_dim = dims
    z, c = place[0], place[3]
    half = v_dim // nc
    for own_core in range(nc):

        @pl.when(c == own_core)
        def _():
            for target, ref in ((own_core, keep), (1 - own_core, give)):
                q, k = ((q1, k1), (q2, k2))[target]
                for b in range(hp):
                    slot = jnp.bitwise_xor(lax.rem(z, hp), b)
                    ref[slot, :, :qk] = q[:, b * qk : (b + 1) * qk]
                    ref[slot, :, qk : 2 * qk] = k[:, b * qk : (b + 1) * qk]
                    low = b * v_dim + target * half
                    ref[slot, :, 2 * qk :] = v[:, low : low + half]


def project_kernel(dims, place, cos_ref, sin_ref, *refs):
    nz, ny, nx, nc, _, depth, qk, windows = dims
    tokens = refs[: nz * nx]
    weights = refs[nz * nx : nz * nx + nz * ny * nc]
    out_ref, acc = refs[nz * nx + nz * ny * nc :]
    z, y = place[0], place[1]
    low, high = windows[0][0], windows[-1][1]
    for r in range(nz):
        for ky in range(ny):
            start = (jnp.bitwise_xor(z, r) * ny + lax.rem(y + ky, ny)) * depth
            cols = pl.ds(pl.multiple_of(start, depth), depth)
            left = jnp.concatenate([t[:, cols] for t in tokens], axis=0)
            for kc in range(nc):
                right = weights[(r * ny + ky) * nc + kc][:, low:high]
                part = jnp.dot(left, right, preferred_element_type=jnp.float32)
                if r or ky:
                    part = part + acc[kc]
                acc[kc] = part
    half = qk // 2
    at = 0
    for first, last, rotated in windows:
        for kc in range(nc):
            value = acc[kc, :, first - low : last - low]
            if rotated:
                a, b = value[:, :half], value[:, half:]
                cos, sin = cos_ref[...], sin_ref[...]
                value = jnp.concatenate([a * cos - b * sin, b * cos + a * sin], axis=1)
            out_ref[:, at : at + last - first] = value.astype(jnp.bfloat16)
            at += last - first


def attend_kernel(dims, place, q_ref, lam_ref, gain_ref, *refs):
    nz, ny, nx, nc, rows, qk, v = dims
    pieces = refs[: ny * nc]
    out_ref, kv_all, s_all = refs[ny * nc :]
    z, y, x, c = (place[i] for i in range(4))
    tile = nx * rows
    block = ny * nc * tile
    half = v // nc
    for ky in range(ny):
        for kc in range(nc):
            piece = pieces[ky * nc + kc]
            slot = lax.rem(y + ky, ny) * nc + lax.rem(c + kc, nc)
            for r in range(nz):
                start = (jnp.bitwise_xor(z, r) * (ny * nc) + slot) * tile
                to = pl.ds(pl.multiple_of(start, tile), tile)
                part = piece[r * tile : (r + 1) * tile, :]
                for m in range(nc):
                    n = (m + kc) % nc
                    kv_all[to, n * qk : (n + 1) * qk] = part[:, m * qk : (m + 1) * qk]
                    kv_all[to, nc * qk + n * half : nc * qk + (n + 1) * half] = part[
                        :, nc * qk + m * half : nc * qk + (m + 1) * half
                    ]

    def offset(index, y_at, c_at):
        x_at = lax.rem(x + index // rows, nx)
        return (y_at * nx + x_at) * nc * rows + c_at * rows + index % rows

    chunk = min(block, 512)
    each = block // chunk
    q_off = offset(lax.broadcasted_iota(jnp.int32, (tile, 1), 0), y, c)
    k_index = lax.broadcasted_iota(jnp.int32, (1, chunk), 1)
    factor = qk ** (-0.5) * LOG2_E

    def key_rows(j):
        return pl.ds(pl.multiple_of(j * chunk, chunk), chunk)

    for t in range(nz):
        q_start = pl.multiple_of(jnp.bitwise_xor(z, t) * tile, tile)
        outs = []
        for m in range(nc):
            q = q_ref[pl.ds(q_start, tile), m * qk : (m + 1) * qk]

            def scores(j, top, masked):
                keys = kv_all[key_rows(j), m * qk : (m + 1) * qk]
                s = lax.dot_general(
                    q, keys, (((1,), (1,)), ((), ())), preferred_element_type=jnp.float32
                )
                if masked:
                    index = k_index + (j - t * each) * chunk
                    slot = index // tile
                    k_off = offset(index % tile, slot // nc, slot % nc)
                    s = jnp.where(k_off <= q_off, s, MASKED)
                s_all[:, key_rows(j)] = s
                return jnp.maximum(top, jnp.max(s, axis=-1, keepdims=True))

            top = jnp.full((tile, 1), MASKED, jnp.float32)
            top = sweep(0, t * each, lambda j, v_: scores(j, v_, False), top)
            top = sweep(t * each, (t + 1) * each, lambda j, v_: scores(j, v_, True), top)

            def gather(j, carry):
                total, acc = carry
                e = jnp.exp2((s_all[:, key_rows(j)] - top) * factor)
                total = total + jnp.sum(e, axis=-1, keepdims=True)
                vals = kv_all[key_rows(j), nc * qk :]
                acc = acc + jnp.dot(
                    e.astype(jnp.bfloat16), vals, preferred_element_type=jnp.float32
                )
                return total, acc

            total, acc = sweep(
                0,
                (t + 1) * each,
                gather,
                (jnp.zeros((tile, 1), jnp.float32), jnp.zeros((tile, v), jnp.float32)),
            )
            outs.append(acc / total)
        one = jnp.where(c == 0, outs[0], outs[1])
        two = jnp.where(c == 0, outs[1], outs[0])
        mixed = one - lam_ref[0] * two
        mixed = jnp.where(
            c == 0, mixed, jnp.concatenate([mixed[:, half:], mixed[:, :half]], axis=1)
        )
        mean = jnp.mean(mixed * mixed, axis=-1, keepdims=True)
        scaled = mixed * lax.rsqrt(mean + EPS_NORM) * gain_ref[...]
        out_ref[t * tile : (t + 1) * tile, :] = scaled.astype(jnp.bfloat16)


def out_kernel(dims, place, *refs):
    nz, ny, nx, nc, hp, v = dims
    chunks = refs[:nz]
    weights = refs[nz : nz + nx * ny * nc]
    out_ref, heads = refs[nz + nx * ny * nc :]
    z, y, c = place[0], place[1], place[3]
    count = chunks[0].shape[0]
    cols = weights[0].shape[1]
    for r in range(nz):
        for kx in range(nx):
            heads[kx, r] = chunks[r][:, kx * v : (kx + 1) * v]
    for ky in range(ny):
        total = jnp.zeros((count, cols), jnp.float32)
        for kx in range(nx):
            for kc in range(nc):
                for b in range(hp):
                    r = jnp.bitwise_xor(lax.rem(c + kc, nc) * hp + b, z)
                    total += jnp.dot(
                        heads[kx, r],
                        weights[(kx * ny + ky) * nc + kc][b * v : (b + 1) * v, :],
                        preferred_element_type=jnp.float32,
                    )
        to = pl.multiple_of(lax.rem(y + ky, ny) * cols, cols)
        out_ref[:, pl.ds(to, cols)] = total.astype(jnp.bfloat16)


def on_device(
    nx,
    tokens,
    query_one,
    query_two,
    key_one,
    key_two,
    value_weight,
    out_weight,
    lambdas,
    head_gain,
):
    sp, tp = lax.axis_size("sp"), lax.axis_size("tp")
    nc = tp // nx
    hp = lambdas.shape[0]
    nz = hp * nc
    ny = sp // nz
    rows = tokens.shape[0]
    span = rows * tp
    depth = query_one.shape[0]
    qk = query_one.shape[1] // hp
    v = value_weight.shape[1] // hp
    half = v // nc
    share = 2 * qk + half
    sp_at, tp_at = lax.axis_index("sp"), lax.axis_index("tp")
    z, y = sp_at // ny, sp_at % ny
    x, c = tp_at // nc, tp_at % nc
    place = jnp.stack([z, y, x, c]).astype(jnp.int32)

    def send(value, where, only=None):
        pairs = []
        for a in range(nz):
            for b in range(ny):
                for d in range(nx):
                    for e in range(nc):
                        if only is not None and a not in only:
                            continue
                        to = where(a, b, d, e)
                        pairs.append(
                            (
                                (a * ny + b) * tp + d * nc + e,
                                (to[0] * ny + to[1]) * tp + to[2] * nc + to[3],
                            )
                        )
        return lax.ppermute(value, ("sp", "tp"), pairs)

    def from_z(value, r):
        return send(value, lambda a, b, d, e: (a ^ r, b, d, e)) if r else value

    def from_y(value, k):
        return send(value, lambda a, b, d, e: (a, (b - k) % ny, d, e)) if k else value

    def from_x(value, k):
        return send(value, lambda a, b, d, e: (a, b, (d - k) % nx, e)) if k else value

    def from_c(value, k):
        return send(value, lambda a, b, d, e: (a, b, d, (e - k) % nc)) if k else value

    if nz == 4:
        mid = (1, 2)
        near = from_z(tokens, 1)
        cross = send(tokens, lambda a, b, d, e: (3 - a, b, d, e), mid)
        out_two = send(cross, lambda a, b, d, e: (a ^ 1, b, d, e), mid)
        mid_two = send(near, lambda a, b, d, e: (3 - a, b, d, e), mid)
        out_three = send(mid_two, lambda a, b, d, e: (a ^ 1, b, d, e), mid)
        in_mid = (z == 1) | (z == 2)
        spans = [
            tokens,
            near,
            jnp.where(in_mid, mid_two, out_two),
            jnp.where(in_mid, cross, out_three),
        ]
    else:
        spans = [from_z(tokens, r) for r in range(nz)]
    token_pieces = [from_x(spans[r], k) for r in range(nz) for k in range(nx)]

    shares = jax.ShapeDtypeStruct((hp, depth, share), jnp.bfloat16)
    keep, give = pl.pallas_call(
        functools.partial(pack_kernel, (nc, hp, qk, v)),
        out_shape=(shares, shares),
        in_specs=[SMEM] + [VMEM] * 5,
        out_specs=(VMEM, VMEM),
        cost_estimate=pl.CostEstimate(
            flops=8 * depth * share * hp, bytes_accessed=8 * depth * share * hp, transcendentals=0
        ),
        name="pack",
    )(place, query_one, query_two, key_one, key_two, value_weight)
    taken = from_c(give, 1)
    weight_pieces = []
    for r in range(nz):
        owner = (z ^ r) // hp
        mine = jnp.where(owner == c, keep[r % hp], taken[r % hp])
        got = from_z(mine, r)
        for ky in range(ny):
            beside = from_y(got, ky)
            for kc in range(nc):
                weight_pieces.append(from_c(beside, kc))

    index = jnp.arange(nz * nx * rows, dtype=jnp.int32)
    at_z = z ^ (index // (nx * rows))
    at_x = (x + (index // rows) % nx) % nx
    positions = (at_z * ny + y) * span + (at_x * nc + c) * rows + index % rows
    turn = qk // 2
    inverse = 1.0 / ROPE_BASE ** (jnp.arange(0, 2 * turn, 2, dtype=jnp.float32) / (2 * turn))
    angles = positions.astype(jnp.float32)[:, None] * inverse[None, :]
    cos_part, sin_part = jnp.cos(angles), jnp.sin(angles)

    total_rows = nz * nx * rows

    def project(windows):
        wide = sum(last - first for first, last, _ in windows)
        return pl.pallas_call(
            functools.partial(project_kernel, (nz, ny, nx, nc, rows, depth, qk, windows)),
            out_shape=jax.ShapeDtypeStruct((total_rows, nc * wide), jnp.bfloat16),
            in_specs=[SMEM] + [VMEM] * (2 + nz * nx + nz * ny * nc),
            out_specs=VMEM,
            scratch_shapes=[pltpu.VMEM((nc, total_rows, wide), jnp.float32)],
            cost_estimate=pl.CostEstimate(
                flops=2 * total_rows * sp * depth * nc * wide,
                bytes_accessed=2 * sp * depth * (total_rows + nc * wide),
                transcendentals=0,
            ),
            compiler_params=room(
                ((total_rows, sp * depth), 2),
                ((sp * depth, nc * share), 2),
                ((total_rows, nc * wide), 6),
            ),
        )(place, cos_part, sin_part, *token_pieces, *weight_pieces)

    kv = project(((qk, 2 * qk, True), (2 * qk, share, False)))
    kv_pieces = []
    for ky in range(ny):
        beside = from_y(kv, ky)
        for kc in range(nc):
            kv_pieces.append(from_c(beside, kc))
    q = project(((0, qk, True),))

    out_pieces = []
    for kx in range(nx):
        over = from_x(out_weight, kx)
        for ky in range(ny):
            beside = from_y(over, ky)
            for kc in range(nc):
                out_pieces.append(from_c(beside, kc))

    lam_all = jnp.stack([from_c(lambdas, k) for k in range(nc)])
    lam = lax.dynamic_slice(lam_all, ((z // hp - c) % nc, z % hp), (1, 1))
    pairs = total_rows * total_rows * ny * nc
    attended = pl.pallas_call(
        functools.partial(attend_kernel, (nz, ny, nx, nc, rows, qk, v)),
        out_shape=jax.ShapeDtypeStruct((total_rows, v), jnp.bfloat16),
        in_specs=[SMEM, VMEM, SMEM, VMEM] + [VMEM] * (ny * nc),
        out_specs=VMEM,
        scratch_shapes=[
            pltpu.VMEM((ny * nc * total_rows, 2 * qk + v), jnp.bfloat16),
            pltpu.VMEM((nx * rows, ny * nc * total_rows), jnp.float32),
        ],
        cost_estimate=pl.CostEstimate(
            flops=4 * pairs * (qk + v),
            bytes_accessed=2 * ny * nc * total_rows * (2 * qk + v),
            transcendentals=2 * pairs,
        ),
        compiler_params=room(
            ((2 * ny * nc * total_rows, 2 * qk + v), 2),
            ((nx * rows, ny * nc * total_rows), 8),
            ((total_rows, v), 4),
        ),
        name="attend",
    )(place, q, lam.reshape(1), head_gain.reshape(1, v), *kv_pieces)

    attended = attended.reshape(nz, nx, rows, v)
    own = jnp.concatenate(
        [from_x(attended[:, (nx - k) % nx], k).reshape(nz * rows, v) for k in range(nx)], axis=1
    )
    chunks = [from_z(own, r) for r in range(nz)]
    cols = ny * out_weight.shape[1]
    result = pl.pallas_call(
        functools.partial(out_kernel, (nz, ny, nx, nc, hp, v)),
        out_shape=jax.ShapeDtypeStruct((nz * rows, cols), jnp.bfloat16),
        in_specs=[SMEM] + [VMEM] * (nz + nx * ny * nc),
        out_specs=VMEM,
        scratch_shapes=[pltpu.VMEM((nx, nz, nz * rows, v), jnp.bfloat16)],
        cost_estimate=pl.CostEstimate(
            flops=2 * nz * rows * nx * nz * v * cols,
            bytes_accessed=2 * nx * nz * v * cols,
            transcendentals=0,
        ),
        compiler_params=room(
            ((nx * nz * v, cols), 2), ((2 * nz * rows, nx * nz * v), 2), ((nz * rows, cols), 6)
        ),
        name="out_project",
    )(place, *chunks, *out_pieces)
    out = jnp.zeros((rows, nz * cols), jnp.bfloat16)
    for r in range(nz):
        mine = lax.dynamic_slice_in_dim(result, (z ^ r) * rows, rows, axis=0)
        out = lax.dynamic_update_slice(out, from_z(mine, r), (0, (z ^ r) * cols))
    return out


def solution(mesh):
    in_specs = (
        P(("sp", "tp"), None),
        P("sp", "tp"),
        P("sp", "tp"),
        P("sp", "tp"),
        P("sp", "tp"),
        P("sp", "tp"),
        P("tp", "sp"),
        P("tp"),
        P(),
    )
    out_specs = P(("sp", "tp"), None)
    nx = 2
    return jax.shard_map(
        functools.partial(on_device, nx),
        mesh=mesh,
        in_specs=in_specs,
        out_specs=out_specs,
        check_vma=False,
    )
```

```python
import functools
import math

import jax
import jax.numpy as jnp
from jax import lax
from jax.experimental import pallas as pl
from jax.experimental.pallas import tpu as pltpu
from jax.sharding import PartitionSpec as P


ROPE_BASE = 500000.0
EPS_NORM = 0.02
MASKED = -1e30
LOG2_E = 1.4426950408889634


SMEM = pl.BlockSpec(memory_space=pltpu.SMEM)
VMEM = pl.BlockSpec(memory_space=pltpu.VMEM)


def room(*shapes):
    held = sum(math.prod(shape) * size for shape, size in shapes)
    return pltpu.CompilerParams(vmem_limit_bytes=min(60 << 20, held + held // 4 + (3 << 20)))


def sweep(low, high, body, carry):
    if high - low <= 4:
        for i in range(low, high):
            carry = body(i, carry)
        return carry
    return lax.fori_loop(low, high, body, carry)


def pack_kernel(dims, place, q1, q2, k1, k2, v, keep, give, keep_q, give_q):
    _, nc, _, hp, qk, v_dim = dims
    z, c = place[0], place[3]
    half = v_dim // nc
    for own_core in range(nc):

        @pl.when(c == own_core)
        def _():
            for target, ref, q_ref in ((own_core, keep, keep_q), (1 - own_core, give, give_q)):
                q, k = ((q1, k1), (q2, k2))[target]
                for b in range(hp):
                    slot = jnp.bitwise_xor(lax.rem(z, hp), b)
                    q_ref[slot] = q[:, b * qk : (b + 1) * qk]
                    ref[slot, :, :qk] = k[:, b * qk : (b + 1) * qk]
                    low = b * v_dim + target * half
                    ref[slot, :, qk:] = v[:, low : low + half]


def project_kernel(dims, place, cos_ref, sin_ref, *refs):
    nz, ny, nx, nc, _, depth, qk, windows, stacked = dims
    tokens = refs[: nz * nx]
    weights = refs[nz * nx : -2]
    out_ref, acc = refs[-2:]
    z, y = place[0], place[1]
    low, high = windows[0][0], windows[-1][1]
    for r in range(nz):
        for ky in range(ny):
            start = (jnp.bitwise_xor(z, r) * ny + lax.rem(y + ky, ny)) * depth
            cols = pl.ds(pl.multiple_of(start, depth), depth)
            left = jnp.concatenate([t[:, cols] for t in tokens], axis=0)
            for kc in range(nc):
                if stacked:
                    right = weights[ky * nc + kc][r * depth : (r + 1) * depth, low:high]
                else:
                    right = weights[(r * ny + ky) * nc + kc][:, low:high]
                part = jnp.dot(left, right, preferred_element_type=jnp.float32)
                if r or ky:
                    part = part + acc[kc]
                acc[kc] = part
    half = qk // 2
    at = 0
    for first, last, rotated in windows:
        for kc in range(nc):
            value = acc[kc, :, first - low : last - low]
            if rotated:
                a, b = value[:, :half], value[:, half:]
                cos, sin = cos_ref[...], sin_ref[...]
                value = jnp.concatenate([a * cos - b * sin, b * cos + a * sin], axis=1)
            out_ref[:, at : at + last - first] = value.astype(jnp.bfloat16)
            at += last - first


def attend_kernel(dims, place, q_ref, lam_own, lam_other, gain_ref, *refs):
    nz, ny, nx, nc, rows, qk, v = dims
    pieces = refs[: ny * nc]
    out_ref, kv_all, s_all = refs[ny * nc :]
    z, y, x, c = (place[i] for i in range(4))
    tile = nx * rows
    block = ny * nc * tile
    half = v // nc
    hp = nz // nc
    lam_at = lax.rem(z, hp)
    lam = jnp.where(z // hp == c, lam_own[lam_at], lam_other[lam_at])
    for ky in range(ny):
        for kc in range(nc):
            piece = pieces[ky * nc + kc]
            slot = lax.rem(y + ky, ny) * nc + lax.rem(c + kc, nc)
            for r in range(nz):
                start = (jnp.bitwise_xor(z, r) * (ny * nc) + slot) * tile
                to = pl.ds(pl.multiple_of(start, tile), tile)
                part = piece[r * tile : (r + 1) * tile, :]
                for m in range(nc):
                    n = (m + kc) % nc
                    kv_all[to, n * qk : (n + 1) * qk] = part[:, m * qk : (m + 1) * qk]
                    kv_all[to, nc * qk + n * half : nc * qk + (n + 1) * half] = part[
                        :, nc * qk + m * half : nc * qk + (m + 1) * half
                    ]

    def offset(index, y_at, c_at):
        x_at = lax.rem(x + index // rows, nx)
        return (y_at * nx + x_at) * nc * rows + c_at * rows + index % rows

    chunk = min(block, 512)
    each = block // chunk
    q_off = offset(lax.broadcasted_iota(jnp.int32, (tile, 1), 0), y, c)
    k_index = lax.broadcasted_iota(jnp.int32, (1, chunk), 1)
    factor = qk ** (-0.5) * LOG2_E

    def key_rows(j):
        return pl.ds(pl.multiple_of(j * chunk, chunk), chunk)

    for t in range(nz):
        q_start = pl.multiple_of(jnp.bitwise_xor(z, t) * tile, tile)
        outs = []
        for m in range(nc):
            q = q_ref[pl.ds(q_start, tile), m * qk : (m + 1) * qk]

            def scores(j, top, masked):
                keys = kv_all[key_rows(j), m * qk : (m + 1) * qk]
                s = lax.dot_general(
                    q, keys, (((1,), (1,)), ((), ())), preferred_element_type=jnp.float32
                )
                if masked:
                    index = k_index + (j - t * each) * chunk
                    slot = index // tile
                    k_off = offset(index % tile, slot // nc, slot % nc)
                    s = jnp.where(k_off <= q_off, s, MASKED)
                s_all[:, key_rows(j)] = s
                return jnp.maximum(top, jnp.max(s, axis=-1, keepdims=True))

            top = jnp.full((tile, 1), MASKED, jnp.float32)
            top = sweep(0, t * each, lambda j, v_: scores(j, v_, False), top)
            top = sweep(t * each, (t + 1) * each, lambda j, v_: scores(j, v_, True), top)

            def gather(j, carry):
                total, acc = carry
                e = jnp.exp2((s_all[:, key_rows(j)] - top) * factor)
                total = total + jnp.sum(e, axis=-1, keepdims=True)
                vals = kv_all[key_rows(j), nc * qk :]
                acc = acc + jnp.dot(
                    e.astype(jnp.bfloat16), vals, preferred_element_type=jnp.float32
                )
                return total, acc

            total, acc = sweep(
                0,
                (t + 1) * each,
                gather,
                (jnp.zeros((tile, 1), jnp.float32), jnp.zeros((tile, v), jnp.float32)),
            )
            outs.append(acc / total)
        one = jnp.where(c == 0, outs[0], outs[1])
        two = jnp.where(c == 0, outs[1], outs[0])
        mixed = one - lam * two
        mixed = jnp.where(
            c == 0, mixed, jnp.concatenate([mixed[:, half:], mixed[:, :half]], axis=1)
        )
        mean = jnp.mean(mixed * mixed, axis=-1, keepdims=True)
        scaled = mixed * lax.rsqrt(mean + EPS_NORM) * gain_ref[...]
        out_ref[t * tile : (t + 1) * tile, :] = scaled.astype(jnp.bfloat16)


def out_kernel(dims, place, *refs):
    nz, ny, nx, nc, hp, v = dims
    chunks = refs[: nx * nz]
    weights = refs[nx * nz : nx * nz + nx * ny * nc]
    out_ref, heads = refs[nx * nz + nx * ny * nc :]
    z, y, c = place[0], place[1], place[3]
    count = chunks[0].shape[0]
    cols = weights[0].shape[1]
    for kx in range(nx):
        for r in range(nz):
            heads[kx, r] = chunks[kx * nz + r][...]
    for ky in range(ny):
        total = jnp.zeros((count, cols), jnp.float32)
        for kx in range(nx):
            for kc in range(nc):
                for b in range(hp):
                    r = jnp.bitwise_xor(lax.rem(c + kc, nc) * hp + b, z)
                    total += jnp.dot(
                        heads[kx, r],
                        weights[(kx * ny + ky) * nc + kc][b * v : (b + 1) * v, :],
                        preferred_element_type=jnp.float32,
                    )
        to = pl.multiple_of(lax.rem(y + ky, ny) * cols, cols)
        out_ref[:, pl.ds(to, cols)] = total.astype(jnp.bfloat16)


def on_device(
    nx,
    tokens,
    query_one,
    query_two,
    key_one,
    key_two,
    value_weight,
    out_weight,
    lambdas,
    head_gain,
):
    sp, tp = lax.axis_size("sp"), lax.axis_size("tp")
    nc = tp // nx
    hp = lambdas.shape[0]
    nz = hp * nc
    ny = sp // nz
    rows = tokens.shape[0]
    span = rows * tp
    depth = query_one.shape[0]
    qk = query_one.shape[1] // hp
    v = value_weight.shape[1] // hp
    half = v // nc
    share = qk + half
    sp_at, tp_at = lax.axis_index("sp"), lax.axis_index("tp")
    z, y = sp_at // ny, sp_at % ny
    x, c = tp_at // nc, tp_at % nc
    place = jnp.stack([z, y, x, c]).astype(jnp.int32)

    def send(value, where, only=None):
        pairs = []
        for a in range(nz):
            for b in range(ny):
                for d in range(nx):
                    for e in range(nc):
                        if only is not None and a not in only:
                            continue
                        to = where(a, b, d, e)
                        pairs.append(
                            (
                                (a * ny + b) * tp + d * nc + e,
                                (to[0] * ny + to[1]) * tp + to[2] * nc + to[3],
                            )
                        )
        return lax.ppermute(value, ("sp", "tp"), pairs)

    def from_z(value, r):
        return send(value, lambda a, b, d, e: (a ^ r, b, d, e)) if r else value

    def from_y(value, k):
        return send(value, lambda a, b, d, e: (a, (b - k) % ny, d, e)) if k else value

    def from_x(value, k):
        return send(value, lambda a, b, d, e: (a, b, (d - k) % nx, e)) if k else value

    def from_c(value, k):
        return send(value, lambda a, b, d, e: (a, b, d, (e - k) % nc)) if k else value

    if nz == 4:
        mid = (1, 2)
        near = from_z(tokens, 1)
        cross = send(tokens, lambda a, b, d, e: (3 - a, b, d, e), mid)
        out_two = send(cross, lambda a, b, d, e: (a ^ 1, b, d, e), mid)
        mid_two = send(near, lambda a, b, d, e: (3 - a, b, d, e), mid)
        out_three = send(mid_two, lambda a, b, d, e: (a ^ 1, b, d, e), mid)
        in_mid = (z == 1) | (z == 2)
        spans = [
            tokens,
            near,
            jnp.where(in_mid, mid_two, out_two),
            jnp.where(in_mid, cross, out_three),
        ]
    else:
        spans = [from_z(tokens, r) for r in range(nz)]
    token_pieces = [from_x(spans[r], k) for r in range(nz) for k in range(nx)]

    shares = jax.ShapeDtypeStruct((hp, depth, share), jnp.bfloat16)
    q_shares = jax.ShapeDtypeStruct((hp, depth, qk), jnp.bfloat16)
    keep, give, keep_q, give_q = pl.pallas_call(
        functools.partial(pack_kernel, (nx, nc, ny, hp, qk, v)),
        out_shape=(shares, shares, q_shares, q_shares),
        in_specs=[SMEM] + [VMEM] * 5,
        out_specs=(VMEM,) * 4,
        cost_estimate=pl.CostEstimate(
            flops=8 * depth * share * hp, bytes_accessed=8 * depth * share * hp, transcendentals=0
        ),
        name="pack",
    )(place, query_one, query_two, key_one, key_two, value_weight)
    taken, taken_q = from_c(give, 1), from_c(give_q, 1)
    weight_pieces, q_rows = [], []
    for r in range(nz):
        own_core = (z ^ r) // hp == c
        got = from_z(jnp.where(own_core, keep[r % hp], taken[r % hp]), r)
        for ky in range(ny):
            beside = from_y(got, ky)
            for kc in range(nc):
                weight_pieces.append(from_c(beside, kc))
    for r in range(nz):
        own_core = (z ^ r) // hp == c
        q_rows.append(from_z(jnp.where(own_core, keep_q[r % hp], taken_q[r % hp]), r))
    q_rows = jnp.concatenate(q_rows, axis=0)
    q_pieces = []
    for ky in range(ny):
        beside = from_y(q_rows, ky)
        for kc in range(nc):
            q_pieces.append(from_c(beside, kc))

    index = jnp.arange(nz * nx * rows, dtype=jnp.int32)
    at_z = z ^ (index // (nx * rows))
    at_x = (x + (index // rows) % nx) % nx
    positions = (at_z * ny + y) * span + (at_x * nc + c) * rows + index % rows
    turn = qk // 2
    inverse = 1.0 / ROPE_BASE ** (jnp.arange(0, 2 * turn, 2, dtype=jnp.float32) / (2 * turn))
    angles = positions.astype(jnp.float32)[:, None] * inverse[None, :]
    cos_part, sin_part = jnp.cos(angles), jnp.sin(angles)

    total_rows = nz * nx * rows

    def project(windows, weights):
        wide = sum(last - first for first, last, _ in windows)
        stacked = len(weights) < nz * ny * nc
        return pl.pallas_call(
            functools.partial(project_kernel, (nz, ny, nx, nc, rows, depth, qk, windows, stacked)),
            out_shape=jax.ShapeDtypeStruct((total_rows, nc * wide), jnp.bfloat16),
            in_specs=[SMEM] + [VMEM] * (2 + nz * nx + len(weights)),
            out_specs=VMEM,
            scratch_shapes=[pltpu.VMEM((nc, total_rows, wide), jnp.float32)],
            cost_estimate=pl.CostEstimate(
                flops=2 * total_rows * sp * depth * nc * wide,
                bytes_accessed=2 * sp * depth * (total_rows + nc * wide),
                transcendentals=0,
            ),
            compiler_params=room(
                ((total_rows, sp * depth), 2),
                ((sp * depth, nc * (share + qk)), 2),
                ((total_rows, nc * wide), 6),
            ),
        )(place, cos_part, sin_part, *token_pieces, *weights)

    kv = project(((0, qk, True), (qk, share, False)), weight_pieces)
    kv_pieces = []
    for ky in range(ny):
        beside = from_y(kv, ky)
        for kc in range(nc):
            kv_pieces.append(from_c(beside, kc))
    q = project(((0, qk, True),), q_pieces)

    out_pieces = []
    for kx in range(nx):
        over = from_x(out_weight, kx)
        for ky in range(ny):
            beside = from_y(over, ky)
            for kc in range(nc):
                out_pieces.append(from_c(beside, kc))

    lam_other = from_c(lambdas, 1)
    pairs = total_rows * total_rows * ny * nc
    attended = pl.pallas_call(
        functools.partial(attend_kernel, (nz, ny, nx, nc, rows, qk, v)),
        out_shape=jax.ShapeDtypeStruct((total_rows, v), jnp.bfloat16),
        in_specs=[SMEM, VMEM, SMEM, SMEM, VMEM] + [VMEM] * (ny * nc),
        out_specs=VMEM,
        scratch_shapes=[
            pltpu.VMEM((ny * nc * total_rows, 2 * qk + v), jnp.bfloat16),
            pltpu.VMEM((nx * rows, ny * nc * total_rows), jnp.float32),
        ],
        cost_estimate=pl.CostEstimate(
            flops=4 * pairs * (qk + v),
            bytes_accessed=2 * ny * nc * total_rows * (2 * qk + v),
            transcendentals=2 * pairs,
        ),
        compiler_params=room(
            ((2 * ny * nc * total_rows, 2 * qk + v), 2),
            ((nx * rows, ny * nc * total_rows), 8),
            ((total_rows, v), 4),
        ),
        name="attend",
    )(place, q, lambdas, lam_other, head_gain.reshape(1, v), *kv_pieces)

    attended = attended.reshape(nz, nx, rows, v)
    chunks = []
    for k in range(nx):
        mine = attended[:, k].reshape(nz * rows, v)
        for r in range(nz):
            chunks.append(
                send(mine, lambda a, b, d, e, k=k, r=r: (a ^ r, b, (d + k) % nx, e))
                if k or r
                else mine
            )
    cols = ny * out_weight.shape[1]
    result = pl.pallas_call(
        functools.partial(out_kernel, (nz, ny, nx, nc, hp, v)),
        out_shape=jax.ShapeDtypeStruct((nz * rows, cols), jnp.bfloat16),
        in_specs=[SMEM] + [VMEM] * (nx * nz + nx * ny * nc),
        out_specs=VMEM,
        scratch_shapes=[pltpu.VMEM((nx, nz, nz * rows, v), jnp.bfloat16)],
        cost_estimate=pl.CostEstimate(
            flops=2 * nz * rows * nx * nz * v * cols,
            bytes_accessed=2 * nx * nz * v * cols,
            transcendentals=0,
        ),
        compiler_params=room(
            ((nx * nz * v, cols), 2), ((2 * nz * rows, nx * nz * v), 2), ((nz * rows, cols), 6)
        ),
        name="out_project",
    )(place, *chunks, *out_pieces)
    out = jnp.zeros((rows, nz * cols), jnp.bfloat16)
    for r in range(nz):
        mine = lax.dynamic_slice_in_dim(result, (z ^ r) * rows, rows, axis=0)
        out = lax.dynamic_update_slice(out, from_z(mine, r), (0, (z ^ r) * cols))
    return out


def solution(mesh):
    in_specs = (
        P(("sp", "tp"), None),
        P("sp", "tp"),
        P("sp", "tp"),
        P("sp", "tp"),
        P("sp", "tp"),
        P("sp", "tp"),
        P("tp", "sp"),
        P("tp"),
        P(),
    )
    out_specs = P(("sp", "tp"), None)
    nx = 2
    return jax.shard_map(
        functools.partial(on_device, nx),
        mesh=mesh,
        in_specs=in_specs,
        out_specs=out_specs,
        check_vma=False,
    )
```

```python
import functools
import math

import jax
import jax.numpy as jnp
from jax import lax
from jax.experimental import pallas as pl
from jax.experimental.pallas import tpu as pltpu
from jax.sharding import PartitionSpec as P


ROPE_BASE = 500000.0
EPS_NORM = 0.02
MASKED = -1e30
LOG2_E = 1.4426950408889634


SMEM = pl.BlockSpec(memory_space=pltpu.SMEM)
VMEM = pl.BlockSpec(memory_space=pltpu.VMEM)


def room(*shapes):
    held = sum(math.prod(shape) * size for shape, size in shapes)
    return pltpu.CompilerParams(vmem_limit_bytes=min(60 << 20, held + held // 4 + (3 << 20)))


def sweep(low, high, body, carry):
    if high - low <= 4:
        for i in range(low, high):
            carry = body(i, carry)
        return carry
    return lax.fori_loop(low, high, body, carry)


def pack_kernel(dims, place, q1, q2, k1, k2, v, keep, give, keep_q, give_q):
    _, nc, _, hp, qk, v_dim = dims
    z, c = place[0], place[3]
    half = v_dim // nc
    for own_core in range(nc):

        @pl.when(c == own_core)
        def _():
            for target, ref, q_ref in ((own_core, keep, keep_q), (1 - own_core, give, give_q)):
                q, k = ((q1, k1), (q2, k2))[target]
                for b in range(hp):
                    slot = jnp.bitwise_xor(lax.rem(z, hp), b)
                    q_ref[slot] = q[:, b * qk : (b + 1) * qk]
                    ref[slot, :, :qk] = k[:, b * qk : (b + 1) * qk]
                    low = b * v_dim + target * half
                    ref[slot, :, qk:] = v[:, low : low + half]


def project_kernel(dims, place, cos_ref, sin_ref, *refs):
    nz, ny, nx, nc, _, depth, qk, windows = dims
    tokens = refs[: nz * nx]
    weights = refs[nz * nx : -2]
    per = nz * ny * nc // len(weights)
    out_ref, acc = refs[-2:]
    z, y = place[0], place[1]
    low, high = windows[0][0], windows[-1][1]
    for r in range(nz):
        for ky in range(ny):
            start = (jnp.bitwise_xor(z, r) * ny + lax.rem(y + ky, ny)) * depth
            cols = pl.ds(pl.multiple_of(start, depth), depth)
            left = jnp.concatenate([t[:, cols] for t in tokens], axis=0)
            for kc in range(nc):
                first = r % per * depth
                right = weights[(r // per * ny + ky) * nc + kc][first : first + depth, low:high]
                part = jnp.dot(left, right, preferred_element_type=jnp.float32)
                if r or ky:
                    part = part + acc[kc]
                acc[kc] = part
    half = qk // 2
    at = 0
    for first, last, rotated in windows:
        for kc in range(nc):
            value = acc[kc, :, first - low : last - low]
            if rotated:
                a, b = value[:, :half], value[:, half:]
                cos, sin = cos_ref[...], sin_ref[...]
                value = jnp.concatenate([a * cos - b * sin, b * cos + a * sin], axis=1)
            out_ref[:, at : at + last - first] = value.astype(jnp.bfloat16)
            at += last - first


def attend_kernel(dims, place, q_ref, lam_own, lam_other, gain_ref, *refs):
    nz, ny, nx, nc, rows, qk, v = dims
    pieces = refs[: ny * nc]
    out_refs, (kv_all, s_all) = refs[ny * nc : -2], refs[-2:]
    z, y, x, c = (place[i] for i in range(4))
    tile = nx * rows
    block = ny * nc * tile
    half = v // nc
    hp = nz // nc
    lam_at = lax.rem(z, hp)
    lam = jnp.where(z // hp == c, lam_own[lam_at], lam_other[lam_at])
    for ky in range(ny):
        for kc in range(nc):
            piece = pieces[ky * nc + kc]
            slot = lax.rem(y + ky, ny) * nc + lax.rem(c + kc, nc)
            for r in range(nz):
                start = (jnp.bitwise_xor(z, r) * (ny * nc) + slot) * tile
                to = pl.ds(pl.multiple_of(start, tile), tile)
                part = piece[r * tile : (r + 1) * tile, :]
                for m in range(nc):
                    n = (m + kc) % nc
                    kv_all[to, n * qk : (n + 1) * qk] = part[:, m * qk : (m + 1) * qk]
                    kv_all[to, nc * qk + n * half : nc * qk + (n + 1) * half] = part[
                        :, nc * qk + m * half : nc * qk + (m + 1) * half
                    ]

    def offset(index, y_at, c_at):
        x_at = lax.rem(x + index // rows, nx)
        return (y_at * nx + x_at) * nc * rows + c_at * rows + index % rows

    chunk = min(block, 512)
    each = block // chunk
    q_off = offset(lax.broadcasted_iota(jnp.int32, (tile, 1), 0), y, c)
    k_index = lax.broadcasted_iota(jnp.int32, (1, chunk), 1)
    factor = qk ** (-0.5) * LOG2_E

    def key_rows(j):
        return pl.ds(pl.multiple_of(j * chunk, chunk), chunk)

    for t in range(nz):
        q_start = pl.multiple_of(jnp.bitwise_xor(z, t) * tile, tile)
        outs = []
        for m in range(nc):
            q = q_ref[pl.ds(q_start, tile), m * qk : (m + 1) * qk]

            def scores(j, top, masked):
                keys = kv_all[key_rows(j), m * qk : (m + 1) * qk]
                s = lax.dot_general(
                    q, keys, (((1,), (1,)), ((), ())), preferred_element_type=jnp.float32
                )
                if masked:
                    index = k_index + (j - t * each) * chunk
                    slot = index // tile
                    k_off = offset(index % tile, slot // nc, slot % nc)
                    s = jnp.where(k_off <= q_off, s, MASKED)
                s_all[:, key_rows(j)] = s
                return jnp.maximum(top, jnp.max(s, axis=-1, keepdims=True))

            top = jnp.full((tile, 1), MASKED, jnp.float32)
            top = sweep(0, t * each, lambda j, v_: scores(j, v_, False), top)
            top = sweep(t * each, (t + 1) * each, lambda j, v_: scores(j, v_, True), top)

            def gather(j, carry):
                total, acc = carry
                e = jnp.exp2((s_all[:, key_rows(j)] - top) * factor)
                total = total + jnp.sum(e, axis=-1, keepdims=True)
                vals = kv_all[key_rows(j), nc * qk :]
                acc = acc + jnp.dot(
                    e.astype(jnp.bfloat16), vals, preferred_element_type=jnp.float32
                )
                return total, acc

            total, acc = sweep(
                0,
                (t + 1) * each,
                gather,
                (jnp.zeros((tile, 1), jnp.float32), jnp.zeros((tile, v), jnp.float32)),
            )
            outs.append(acc / total)
        one = jnp.where(c == 0, outs[0], outs[1])
        two = jnp.where(c == 0, outs[1], outs[0])
        mixed = one - lam * two
        mixed = jnp.where(
            c == 0, mixed, jnp.concatenate([mixed[:, half:], mixed[:, :half]], axis=1)
        )
        mean = jnp.mean(mixed * mixed, axis=-1, keepdims=True)
        scaled = mixed * lax.rsqrt(mean + EPS_NORM) * gain_ref[...]
        done = scaled.astype(jnp.bfloat16)
        for k in range(nx):
            out_refs[k][t * rows : (t + 1) * rows, :] = done[k * rows : (k + 1) * rows, :]


def out_kernel(dims, place, *refs):
    nz, ny, nx, nc, hp, v = dims
    chunks = refs[: nx * nz]
    weights = refs[nx * nz : nx * nz + nx * ny * nc]
    out_ref, heads = refs[nx * nz + nx * ny * nc :]
    z, y, c = place[0], place[1], place[3]
    count = chunks[0].shape[0]
    cols = weights[0].shape[1]
    for kx in range(nx):
        for r in range(nz):
            heads[kx, r] = chunks[kx * nz + r][...]
    for ky in range(ny):
        total = jnp.zeros((count, cols), jnp.float32)
        for kx in range(nx):
            for kc in range(nc):
                for b in range(hp):
                    r = jnp.bitwise_xor(lax.rem(c + kc, nc) * hp + b, z)
                    total += jnp.dot(
                        heads[kx, r],
                        weights[(kx * ny + ky) * nc + kc][b * v : (b + 1) * v, :],
                        preferred_element_type=jnp.float32,
                    )
        to = pl.multiple_of(lax.rem(y + ky, ny) * cols, cols)
        out_ref[:, pl.ds(to, cols)] = total.astype(jnp.bfloat16)


def on_device(
    nx,
    tokens,
    query_one,
    query_two,
    key_one,
    key_two,
    value_weight,
    out_weight,
    lambdas,
    head_gain,
):
    sp, tp = lax.axis_size("sp"), lax.axis_size("tp")
    nc = tp // nx
    hp = lambdas.shape[0]
    nz = hp * nc
    ny = sp // nz
    rows = tokens.shape[0]
    span = rows * tp
    depth = query_one.shape[0]
    qk = query_one.shape[1] // hp
    v = value_weight.shape[1] // hp
    half = v // nc
    share = qk + half
    sp_at, tp_at = lax.axis_index("sp"), lax.axis_index("tp")
    z, y = sp_at // ny, sp_at % ny
    x, c = tp_at // nc, tp_at % nc
    place = jnp.stack([z, y, x, c]).astype(jnp.int32)

    def send(value, where, only=None):
        pairs = []
        for a in range(nz):
            for b in range(ny):
                for d in range(nx):
                    for e in range(nc):
                        if only is not None and a not in only:
                            continue
                        to = where(a, b, d, e)
                        pairs.append(
                            (
                                (a * ny + b) * tp + d * nc + e,
                                (to[0] * ny + to[1]) * tp + to[2] * nc + to[3],
                            )
                        )
        return lax.ppermute(value, ("sp", "tp"), pairs)

    def from_z(value, r):
        return send(value, lambda a, b, d, e: (a ^ r, b, d, e)) if r else value

    def from_y(value, k):
        return send(value, lambda a, b, d, e: (a, (b - k) % ny, d, e)) if k else value

    def from_x(value, k):
        return send(value, lambda a, b, d, e: (a, b, (d - k) % nx, e)) if k else value

    def from_c(value, k):
        return send(value, lambda a, b, d, e: (a, b, d, (e - k) % nc)) if k else value

    if nz == 4:
        mid = (1, 2)
        near = from_z(tokens, 1)
        cross = send(tokens, lambda a, b, d, e: (3 - a, b, d, e), mid)
        out_two = send(cross, lambda a, b, d, e: (a ^ 1, b, d, e), mid)
        mid_two = send(near, lambda a, b, d, e: (3 - a, b, d, e), mid)
        out_three = send(mid_two, lambda a, b, d, e: (a ^ 1, b, d, e), mid)
        in_mid = (z == 1) | (z == 2)
        spans = [
            tokens,
            near,
            jnp.where(in_mid, mid_two, out_two),
            jnp.where(in_mid, cross, out_three),
        ]
    else:
        spans = [from_z(tokens, r) for r in range(nz)]
    token_pieces = [from_x(spans[r], k) for r in range(nz) for k in range(nx)]

    shares = jax.ShapeDtypeStruct((hp, depth, share), jnp.bfloat16)
    q_shares = jax.ShapeDtypeStruct((hp, depth, qk), jnp.bfloat16)
    keep, give, keep_q, give_q = pl.pallas_call(
        functools.partial(pack_kernel, (nx, nc, ny, hp, qk, v)),
        out_shape=(shares, shares, q_shares, q_shares),
        in_specs=[SMEM] + [VMEM] * 5,
        out_specs=(VMEM,) * 4,
        cost_estimate=pl.CostEstimate(
            flops=8 * depth * share * hp, bytes_accessed=8 * depth * share * hp, transcendentals=0
        ),
        name="pack",
    )(place, query_one, query_two, key_one, key_two, value_weight)
    taken, taken_q = from_c(give, 1), from_c(give_q, 1)
    weight_pieces, q_rows = [], []
    for r in range(nz):
        own_core = (z ^ r) // hp == c
        got = from_z(jnp.where(own_core, keep[r % hp], taken[r % hp]), r)
        for ky in range(ny):
            beside = from_y(got, ky)
            for kc in range(nc):
                weight_pieces.append(from_c(beside, kc))
    for r in range(nz):
        own_core = (z ^ r) // hp == c
        q_rows.append(from_z(jnp.where(own_core, keep_q[r % hp], taken_q[r % hp]), r))
    q_pieces = []
    for g in range(2):
        group = jnp.concatenate(q_rows[g * nz // 2 : (g + 1) * nz // 2], axis=0)
        for ky in range(ny):
            beside = from_y(group, ky)
            for kc in range(nc):
                q_pieces.append(from_c(beside, kc))

    index = jnp.arange(nz * nx * rows, dtype=jnp.int32)
    at_z = z ^ (index // (nx * rows))
    at_x = (x + (index // rows) % nx) % nx
    positions = (at_z * ny + y) * span + (at_x * nc + c) * rows + index % rows
    turn = qk // 2
    inverse = 1.0 / ROPE_BASE ** (jnp.arange(0, 2 * turn, 2, dtype=jnp.float32) / (2 * turn))
    angles = positions.astype(jnp.float32)[:, None] * inverse[None, :]
    cos_part, sin_part = jnp.cos(angles), jnp.sin(angles)

    total_rows = nz * nx * rows

    def project(windows, weights):
        wide = sum(last - first for first, last, _ in windows)
        return pl.pallas_call(
            functools.partial(project_kernel, (nz, ny, nx, nc, rows, depth, qk, windows)),
            out_shape=jax.ShapeDtypeStruct((total_rows, nc * wide), jnp.bfloat16),
            in_specs=[SMEM] + [VMEM] * (2 + nz * nx + len(weights)),
            out_specs=VMEM,
            scratch_shapes=[pltpu.VMEM((nc, total_rows, wide), jnp.float32)],
            cost_estimate=pl.CostEstimate(
                flops=2 * total_rows * sp * depth * nc * wide,
                bytes_accessed=2 * sp * depth * (total_rows + nc * wide),
                transcendentals=0,
            ),
            compiler_params=room(
                ((total_rows, sp * depth), 2),
                ((sp * depth, nc * (share + qk)), 2),
                ((total_rows, nc * wide), 6),
            ),
        )(place, cos_part, sin_part, *token_pieces, *weights)

    kv = project(((0, qk, True), (qk, share, False)), weight_pieces)
    kv_pieces = []
    for ky in range(ny):
        beside = from_y(kv, ky)
        for kc in range(nc):
            kv_pieces.append(from_c(beside, kc))
    q = project(((0, qk, True),), q_pieces)

    out_pieces = []
    for kx in range(nx):
        over = from_x(out_weight, kx)
        for ky in range(ny):
            beside = from_y(over, ky)
            for kc in range(nc):
                out_pieces.append(from_c(beside, kc))

    lam_other = from_c(lambdas, 1)
    pairs = total_rows * total_rows * ny * nc
    attended = pl.pallas_call(
        functools.partial(attend_kernel, (nz, ny, nx, nc, rows, qk, v)),
        out_shape=(jax.ShapeDtypeStruct((nz * rows, v), jnp.bfloat16),) * nx,
        in_specs=[SMEM, VMEM, SMEM, SMEM, VMEM] + [VMEM] * (ny * nc),
        out_specs=(VMEM,) * nx,
        scratch_shapes=[
            pltpu.VMEM((ny * nc * total_rows, 2 * qk + v), jnp.bfloat16),
            pltpu.VMEM((nx * rows, ny * nc * total_rows), jnp.float32),
        ],
        cost_estimate=pl.CostEstimate(
            flops=4 * pairs * (qk + v),
            bytes_accessed=2 * ny * nc * total_rows * (2 * qk + v),
            transcendentals=2 * pairs,
        ),
        compiler_params=room(
            ((2 * ny * nc * total_rows, 2 * qk + v), 2),
            ((nx * rows, ny * nc * total_rows), 8),
            ((total_rows, v), 4),
        ),
        name="attend",
    )(place, q, lambdas, lam_other, head_gain.reshape(1, v), *kv_pieces)

    chunks = []
    for k in range(nx):
        mine = attended[k]
        for r in range(nz):
            chunks.append(
                send(mine, lambda a, b, d, e, k=k, r=r: (a ^ r, b, (d + k) % nx, e))
                if k or r
                else mine
            )
    cols = ny * out_weight.shape[1]
    result = pl.pallas_call(
        functools.partial(out_kernel, (nz, ny, nx, nc, hp, v)),
        out_shape=jax.ShapeDtypeStruct((nz * rows, cols), jnp.bfloat16),
        in_specs=[SMEM] + [VMEM] * (nx * nz + nx * ny * nc),
        out_specs=VMEM,
        scratch_shapes=[pltpu.VMEM((nx, nz, nz * rows, v), jnp.bfloat16)],
        cost_estimate=pl.CostEstimate(
            flops=2 * nz * rows * nx * nz * v * cols,
            bytes_accessed=2 * nx * nz * v * cols,
            transcendentals=0,
        ),
        compiler_params=room(
            ((nx * nz * v, cols), 2), ((2 * nz * rows, nx * nz * v), 2), ((nz * rows, cols), 6)
        ),
        name="out_project",
    )(place, *chunks, *out_pieces)
    out = jnp.zeros((rows, nz * cols), jnp.bfloat16)
    for r in range(nz):
        mine = lax.dynamic_slice_in_dim(result, (z ^ r) * rows, rows, axis=0)
        out = lax.dynamic_update_slice(out, from_z(mine, r), (0, (z ^ r) * cols))
    return out


def solution(mesh):
    in_specs = (
        P(("sp", "tp"), None),
        P("sp", "tp"),
        P("sp", "tp"),
        P("sp", "tp"),
        P("sp", "tp"),
        P("sp", "tp"),
        P("tp", "sp"),
        P("tp"),
        P(),
    )
    out_specs = P(("sp", "tp"), None)
    nx = 2
    return jax.shard_map(
        functools.partial(on_device, nx),
        mesh=mesh,
        in_specs=in_specs,
        out_specs=out_specs,
        check_vma=False,
    )
```
